32 devices in a mesh: fs: 8 (over z, x), tp: 4 (over y, core).
Axes of the slice: x: 2, y: 2, z: 4, core: 2. Of those that a mesh axis runs over, the one named last changes fastest.
Arguments:
- tokens: bfloat16 [6144, 2048], P('fs', 'tp'), may hold values from -6 to 6
- ffn_one_gain: float32 [2048], replicated, may hold values from 0.1 to 1.9
- ffn_one_gate: bfloat16 [2048, 5632], P('fs', 'tp'), may hold values from -0.125 to 0.125
- ffn_one_up: bfloat16 [2048, 5632], P('fs', 'tp'), may hold values from -0.125 to 0.125
- ffn_one_down: bfloat16 [5632, 2048], P('tp', 'fs'), may hold values from -0.078125 to 0.078125
- mix_gain: float32 [2048], replicated, may hold values from 0.1 to 1.9
- conv_value: bfloat16 [2048, 1024], P('fs', 'tp'), may hold values from -0.125 to 0.125
- conv_gate: bfloat16 [2048, 1024], P('fs', 'tp'), may hold values from -0.125 to 0.125
- conv_kernel: float32 [31, 1024], P(None, 'tp'), may hold values from -15 to 15
- conv_ln_gain: float32 [1024], P('tp'), may hold values from 0.1 to 1.9
- conv_out: bfloat16 [1024, 2048], P('tp', 'fs'), may hold values from -0.1875 to 0.1875
- ffn_two_gain: float32 [2048], replicated, may hold values from 0.1 to 1.9
- ffn_two_gate: bfloat16 [2048, 5632], P('fs', 'tp'), may hold values from -0.125 to 0.125
- ffn_two_up: bfloat16 [2048, 5632], P('fs', 'tp'), may hold values from -0.125 to 0.125
- ffn_two_down: bfloat16 [5632, 2048], P('tp', 'fs'), may hold values from -0.078125 to 0.078125
Outputs:
- layer_out: bfloat16 [6144, 2048], P('fs', 'tp')
The draws below stay inside these ranges and needn't reach their ends.
All inputs are finite; a program needn't handle non-finite values.
Results may differ from the reference program's by a relative error of at most 0.017.
Values may be sent and summed in bfloat16 or wider, within the bound.
A program may use at most 128 MiB of HBM per device.

```python
import jax
import jax.numpy as jnp
from jax import lax

D = 2048
FF = 5632
CONV = 1024
KW = 31
TOK_DEV = 768
TOKENS = 6144
N_FS = 8
N_TP = 4


def draw_conv_kernel(key, part):
    first_key, second_key = jax.random.split(jax.random.fold_in(key, 7))
    base = jnp.clip(jax.random.normal(first_key, (KW, CONV), jnp.float32), -4.0, 4.0) / jnp.sqrt(jnp.float32(KW))
    position = jnp.arange(CONV, dtype=jnp.float32) / jnp.float32(max(CONV - 1, 1))
    rising = 3.0 ** position * jax.random.uniform(second_key, (CONV,), jnp.float32, 0.7, 1.4)
    return base * rising[None, :]


def shard_levels(key, extent, cuts, least, high):
    factor_of, own = 1.0, jax.random.fold_in(key, 6)
    for dim, shards_of in cuts:
        heights = jnp.exp(jax.random.uniform(jax.random.fold_in(own, dim), (shards_of,), jnp.float32, least / len(cuts), high / len(cuts)))
        factor_of = factor_of * jnp.repeat(heights, extent[dim] // shards_of).reshape([-1 if axis == dim else 1 for axis in range(len(extent))])
    return factor_of


def scatter_about(stream_key, dims, width, bound, shards=(), held_as=jnp.bfloat16):
    entries = jax.random.normal(stream_key, dims, jnp.float32) * width
    if len(shards) > 0:
        entries = shard_levels(stream_key, dims, shards, -0.22, 0.18) * entries
    return jnp.clip(entries, min=-bound, max=bound).astype(held_as)


def setup_inputs(seed: int = 0) -> dict:
    key_of = jax.random.split(jax.random.key(seed), 16)
    tokens = scatter_about(key_of[0], (TOKENS, D), 1.0, 6.0, ((0, 8), (1, 4)))
    ffn_one_gain = jnp.clip(1.0 + 0.18 * jax.random.normal(key_of[1], (D,), jnp.float32), 0.1, 1.9)
    ffn_one_gate = scatter_about(key_of[2], (D, FF), D ** -0.5, 0.125, ((0, 8), (1, 4)))
    ffn_one_up = scatter_about(key_of[3], (D, FF), D ** -0.5, 0.125, ((0, 8), (1, 4)))
    ffn_one_down = scatter_about(key_of[4], (FF, D), FF ** -0.5, 0.078125, ((0, 4), (1, 8)))
    mix_gain = jnp.clip(1.0 + 0.18 * jax.random.normal(key_of[5], (D,), jnp.float32), 0.1, 1.9)
    conv_value = scatter_about(key_of[6], (D, CONV), D ** -0.5, 0.125, ((0, 8), (1, 4)))
    conv_gate = scatter_about(key_of[7], (D, CONV), D ** -0.5, 0.125, ((0, 8), (1, 4)))
    conv_kernel = draw_conv_kernel(jax.random.fold_in(key_of[15], 71), 0)
    conv_ln_gain = jnp.clip(1.0 + 0.18 * jax.random.normal(key_of[9], (CONV,), jnp.float32), 0.1, 1.9)
    conv_out = scatter_about(key_of[10], (CONV, D), CONV ** -0.5, 0.1875, ((0, 4), (1, 8)))
    ffn_two_gain = jnp.clip(1.0 + 0.18 * jax.random.normal(key_of[11], (D,), jnp.float32), 0.1, 1.9)
    ffn_two_gate = scatter_about(key_of[12], (D, FF), D ** -0.5, 0.125, ((0, 8), (1, 4)))
    ffn_two_up = scatter_about(key_of[13], (D, FF), D ** -0.5, 0.125, ((0, 8), (1, 4)))
    ffn_two_down = scatter_about(key_of[14], (FF, D), FF ** -0.5, 0.078125, ((0, 4), (1, 8)))
    return dict(tokens=tokens, ffn_one_gain=ffn_one_gain, ffn_one_gate=ffn_one_gate, ffn_one_up=ffn_one_up, ffn_one_down=ffn_one_down, mix_gain=mix_gain, conv_value=conv_value, conv_gate=conv_gate, conv_kernel=conv_kernel, conv_ln_gain=conv_ln_gain, conv_out=conv_out, ffn_two_gain=ffn_two_gain, ffn_two_gate=ffn_two_gate, ffn_two_up=ffn_two_up, ffn_two_down=ffn_two_down)


def rms_rows(rows_in, gain_vec):
    values = rows_in.astype(jnp.float32)
    scaled = values * lax.rsqrt(lax.optimization_barrier(jnp.mean(values * values, axis=-1, keepdims=True)) + 1e-06) * gain_vec
    return scaled.astype(jnp.bfloat16)

def block_sum(hidden, weight, blocks):
    span_width = hidden.shape[1] // blocks
    summed = jnp.zeros((hidden.shape[0], weight.shape[1]), jnp.float32)
    for block_index in range(blocks):
        lower = block_index * span_width
        partial_value = jnp.dot(hidden[:, lower:lower + span_width], weight[lower:lower + span_width], preferred_element_type=jnp.float32).astype(jnp.bfloat16)
        summed = summed + lax.optimization_barrier(partial_value).astype(jnp.float32)
    return summed

def half_ffn(residual, gain_vec, w_gate, w_up, w_down):
    normed = rms_rows(residual, gain_vec)
    gate_pre = jnp.dot(normed, w_gate, preferred_element_type=jnp.float32)
    up_pre = jnp.dot(normed, w_up, preferred_element_type=jnp.float32)
    hidden = (jax.nn.silu(gate_pre) * up_pre).astype(jnp.bfloat16)
    summed = block_sum(hidden, w_down, N_TP)
    return (residual.astype(jnp.float32) + 0.5 * summed).astype(jnp.bfloat16)

def conv_module(residual, mix_gain, conv_value, conv_gate, conv_kernel, conv_ln_gain, conv_out):
    normed = rms_rows(residual, mix_gain)
    value_pre = jnp.dot(normed, conv_value, preferred_element_type=jnp.float32)
    gate_pre = jnp.dot(normed, conv_gate, preferred_element_type=jnp.float32)
    gated_lin = value_pre * jax.nn.sigmoid(gate_pre)
    sequences = gated_lin.reshape(N_FS, TOK_DEV, CONV)
    half_span = KW // 2
    convolved = lax.conv_general_dilated(sequences, conv_kernel[:, None, :], (1,), [(half_span, half_span)], dimension_numbers=('NWC', 'WIO', 'NWC'), feature_group_count=CONV, precision=lax.Precision.HIGHEST).reshape(N_FS * TOK_DEV, CONV)
    mean_val = lax.optimization_barrier(jnp.sum(convolved, axis=1, keepdims=True)) / CONV
    sq_mean = lax.optimization_barrier(jnp.sum(convolved * convolved, axis=1, keepdims=True)) / CONV
    varied = sq_mean - mean_val * mean_val
    active = jax.nn.silu((convolved - mean_val) * lax.rsqrt(varied + 1e-05) * conv_ln_gain).astype(jnp.bfloat16)
    summed = block_sum(active, conv_out, N_TP)
    return (residual.astype(jnp.float32) + summed).astype(jnp.bfloat16)

def reference(tokens, ffn_one_gain, ffn_one_gate, ffn_one_up, ffn_one_down, mix_gain, conv_value, conv_gate, conv_kernel, conv_ln_gain, conv_out, ffn_two_gain, ffn_two_gate, ffn_two_up, ffn_two_down):
    stream = half_ffn(tokens, ffn_one_gain, ffn_one_gate, ffn_one_up, ffn_one_down)
    stream = conv_module(stream, mix_gain, conv_value, conv_gate, conv_kernel, conv_ln_gain, conv_out)
    return half_ffn(stream, ffn_two_gain, ffn_two_gate, ffn_two_up, ffn_two_down)
```

```python
from functools import partial

import jax
import jax.numpy as jnp
from jax import lax
from jax.sharding import PartitionSpec as P


def rms_rows(rows_in, gain_vec):
    values = rows_in.astype(jnp.float32)
    scaled = (
        values * lax.rsqrt(jnp.mean(values * values, axis=-1, keepdims=True) + 1e-06) * gain_vec
    )
    return scaled.astype(jnp.bfloat16)


def split_fs():
    total = lax.axis_size("fs")
    inner = 1
    while total % (inner * 2) == 0 and (inner * 2) ** 2 <= total:
        inner *= 2
    return total // inner, inner


def spread_blocks(shard):
    outer, inner = split_fs()
    me = lax.axis_index("fs")
    mine_z, mine_x = me // inner, me % inner
    held = [shard]
    for hop in range(1, outer):
        pairs = [
            (z * inner + x, ((z + hop) % outer) * inner + x)
            for z in range(outer)
            for x in range(inner)
        ]
        held.append(lax.ppermute(shard, "fs", pairs))
    blocks = []
    for hop, block in enumerate(held):
        blocks.append((((mine_z - hop) % outer) * inner + mine_x, block))
        for step in range(1, inner):
            pairs = [
                (z * inner + x, z * inner + (x + step) % inner)
                for z in range(outer)
                for x in range(inner)
            ]
            owner = ((mine_z - hop) % outer) * inner + (mine_x - step) % inner
            blocks.append((owner, lax.ppermute(block, "fs", pairs)))
    return blocks


def place_blocks(blocks, axis):
    shape = list(blocks[0][1].shape)
    width = shape[axis]
    shape[axis] = width * len(blocks)
    whole = jnp.zeros(shape, blocks[0][1].dtype)
    for owner, block in blocks:
        whole = lax.dynamic_update_slice_in_dim(whole, block, owner * width, axis)
    return whole


def down_product(hidden, blocks):
    return place_blocks(
        [
            (
                owner,
                jnp.dot(hidden, block, preferred_element_type=jnp.float32).astype(jnp.bfloat16),
            )
            for owner, block in blocks
        ],
        1,
    )


def ffn_terms(full_rows, gain_vec, gate_blocks, up_blocks, down_blocks):
    normed = rms_rows(full_rows, gain_vec)
    gate_pre = jnp.dot(normed, place_blocks(gate_blocks, 0), preferred_element_type=jnp.float32)
    up_pre = jnp.dot(normed, place_blocks(up_blocks, 0), preferred_element_type=jnp.float32)
    hidden = (jax.nn.silu(gate_pre) * up_pre).astype(jnp.bfloat16)
    return down_product(hidden, down_blocks)


def conv_terms(full_rows, mix_gain, conv_blocks, conv_kernel, conv_ln_gain):
    normed = rms_rows(full_rows, mix_gain)
    value_whole = place_blocks([(owner, block[0]) for owner, block in conv_blocks], 0)
    gate_whole = place_blocks([(owner, block[1]) for owner, block in conv_blocks], 0)
    value_pre = jnp.dot(normed, value_whole, preferred_element_type=jnp.float32)
    gate_pre = jnp.dot(normed, gate_whole, preferred_element_type=jnp.float32)
    gated_lin = value_pre * jax.nn.sigmoid(gate_pre)
    half_span = conv_kernel.shape[0] // 2
    convolved = lax.conv_general_dilated(
        gated_lin[None],
        conv_kernel[:, None, :],
        (1,),
        [(half_span, half_span)],
        dimension_numbers=("NWC", "WIO", "NWC"),
        feature_group_count=gated_lin.shape[1],
        precision=lax.Precision.HIGHEST,
    )[0]
    sum_one, sum_two = lax.psum(
        (jnp.sum(convolved, axis=1), jnp.sum(convolved * convolved, axis=1)), "tp"
    )
    channels = convolved.shape[1] * lax.axis_size("tp")
    mean_val = (sum_one / channels)[:, None]
    varied = (sum_two / channels)[:, None] - mean_val * mean_val
    active = jax.nn.silu((convolved - mean_val) * lax.rsqrt(varied + 1e-05) * conv_ln_gain).astype(
        jnp.bfloat16
    )
    out_whole = place_blocks([(owner, block[2]) for owner, block in conv_blocks], 0)
    return jnp.einsum("tc,dc->td", active, out_whole, preferred_element_type=jnp.float32)


def keep_features(terms):
    outer = lax.axis_size("tp") // 2
    width = terms.shape[1] // (2 * outer)
    me = lax.axis_index("tp")
    mine_y, core = me // 2, me % 2

    def piece(y, half):
        return lax.dynamic_slice_in_dim(terms, (y * 2 + half) * width, width, 1)

    swap = [(d, d ^ 1) for d in range(2 * outer)]
    halves = []
    for hop in range(outer):
        target = (mine_y + hop) % outer
        other = lax.ppermute(piece(target, 1 - core), "tp", swap)
        halves.append(piece(target, core).astype(jnp.float32) + other.astype(jnp.float32))
    total = halves[0]
    for hop in range(1, outer):
        pairs = [
            (y * 2 + half, ((y + hop) % outer) * 2 + half)
            for y in range(outer)
            for half in range(2)
        ]
        arrived = lax.ppermute(halves[hop].astype(jnp.bfloat16), "tp", pairs)
        total = total + arrived.astype(jnp.float32)
    return total


def per_device(
    tokens,
    ffn_one_gain,
    ffn_one_gate,
    ffn_one_up,
    ffn_one_down,
    mix_gain,
    conv_value,
    conv_gate,
    conv_kernel,
    conv_ln_gain,
    conv_out,
    ffn_two_gain,
    ffn_two_gate,
    ffn_two_up,
    ffn_two_down,
):
    conv_pack = jnp.stack((conv_value, conv_gate, conv_out.T))
    sublayers = [
        (
            partial(
                ffn_terms,
                gain_vec=ffn_one_gain,
                gate_blocks=spread_blocks(ffn_one_gate),
                up_blocks=spread_blocks(ffn_one_up),
                down_blocks=spread_blocks(ffn_one_down),
            ),
            0.5,
        ),
        (
            partial(
                conv_terms,
                mix_gain=mix_gain,
                conv_blocks=spread_blocks(conv_pack),
                conv_kernel=conv_kernel,
                conv_ln_gain=conv_ln_gain,
            ),
            1.0,
        ),
        (
            partial(
                ffn_terms,
                gain_vec=ffn_two_gain,
                gate_blocks=spread_blocks(ffn_two_gate),
                up_blocks=spread_blocks(ffn_two_up),
                down_blocks=spread_blocks(ffn_two_down),
            ),
            0.5,
        ),
    ]
    current = tokens
    for sublayer, factor in sublayers:
        full_rows = lax.all_gather(current, "tp", axis=1, tiled=True)
        run = sublayer
        summed = keep_features(run(full_rows).astype(jnp.bfloat16))
        current = (current.astype(jnp.float32) + factor * summed).astype(jnp.bfloat16)
    return current


def solution(mesh):
    in_specs = (
        P("fs", "tp"),
        P(),
        P("fs", "tp"),
        P("fs", "tp"),
        P("tp", "fs"),
        P(),
        P("fs", "tp"),
        P("fs", "tp"),
        P(None, "tp"),
        P("tp"),
        P("tp", "fs"),
        P(),
        P("fs", "tp"),
        P("fs", "tp"),
        P("tp", "fs"),
    )
    out_specs = P("fs", "tp")
    return jax.shard_map(
        per_device, mesh=mesh, in_specs=in_specs, out_specs=out_specs, check_vma=False
    )
```
